32 devices in a mesh: rep: 2 (over y), fs: 4 (over z), tp: 4 (over x, core).
Axes of the slice: x: 2, y: 2, z: 4, core: 2. Of those that a mesh axis runs over, the one named last changes fastest.
Arguments:
- gate_pre: bfloat16 [8192, 3072], P(('rep', 'fs'), 'tp'), may hold values from -6 to 6
- up_pre: bfloat16 [8192, 3072], P(('rep', 'fs'), 'tp'), may hold values from -6 to 6
- out_grad: bfloat16 [8192, 2048], P(('rep', 'fs')), may hold values from -8 to 8
- w_down: bfloat16 [3072, 2048], P('tp', 'fs'), may hold values from -0.109375 to 0.109375
Outputs:
- d_gate: bfloat16 [8192, 3072], P(('rep', 'fs'), 'tp')
- d_up: bfloat16 [8192, 3072], P(('rep', 'fs'), 'tp')
- grad_down: float32 [3072, 2048], P('tp', 'fs')
- row_energy: float32 [3072], P('tp')
The draws below stay inside these ranges and needn't reach their ends.
All inputs are finite; a program needn't handle non-finite values.
Results may differ from the reference program's by a relative error of at most 0.0034.
Values may be sent and summed in bfloat16 or wider, within the bound.
A program may use at most 64 MiB of HBM per device.

```python
import jax
import jax.numpy as jnp
from jax import lax

D = 2048
FF = 3072
TOK_DEV = 1024
TOKENS = 8192


def raised(result, stream_key, source, target, shards_of, factor):
    def block_of(dim):
        return (jnp.arange(result.shape[dim]) // (result.shape[dim] // shards_of)).reshape((-1,) + (1,) * (result.ndim - 1 - dim))

    first = jax.random.permutation(stream_key, shards_of)[block_of(target)]
    second = (block_of(target) + shards_of // 2) % shards_of
    return jnp.where((block_of(source) == first) | (block_of(source) == second), factor * result, result)


def shard_levels(stream_key, dims, shards, least, top_value):
    factor_of = 1.0
    for axis_at, blocks in shards:
        steps = jax.random.uniform(jax.random.fold_in(jax.random.fold_in(stream_key, 6), axis_at), (blocks,), jnp.float32, least / len(shards), top_value / len(shards))
        factor_of = factor_of * jnp.repeat(jnp.exp(steps), dims[axis_at] // blocks).reshape((-1,) + (1,) * (len(dims) - 1 - axis_at))
    return factor_of


def noise(own_key, extent, deviation, reach, pieces=(), held_as=jnp.bfloat16):
    array = deviation * jax.random.normal(own_key, extent, jnp.float32)
    if pieces:
        array = array * shard_levels(own_key, extent, pieces, -0.22, 0.18)
    return jnp.clip(array, -reach, reach).astype(held_as)


def bell_draw_with(key, extent, spread, reach, split, heavy, dtype=jnp.bfloat16):
    values = spread * jax.random.normal(key, extent, jnp.float32)
    if split:
        values = values * shard_levels(key, extent, split, -0.22, 0.18)
    return jnp.clip(raised(values, jax.random.fold_in(key, 3), *heavy), -reach, reach).astype(dtype)


def setup_inputs(seed: int = 0) -> dict:
    key_of = jax.random.split(jax.random.key(seed), 5)
    return {
        "gate_pre": noise(key_of[0], (TOKENS, FF), 1.0, 6.0, ((0, 8), (1, 4))),
        "up_pre": noise(key_of[1], (TOKENS, FF), 1.0, 6.0, ((0, 8), (1, 4))),
        "out_grad": bell_draw_with(key_of[2], (TOKENS, D), 1.0, 8.0, ((0, 8),), (0, 1, 8, 2.0)),
        "w_down": noise(key_of[3], (FF, D), FF ** -0.5, 0.109375, ((0, 4), (1, 4))),
    }


def reference(gate_pre, up_pre, out_grad, w_down):
    blocks = TOKENS // TOK_DEV
    gate_blocks = gate_pre.reshape(blocks, TOK_DEV, FF)
    up_blocks = up_pre.reshape(blocks, TOK_DEV, FF)
    grad_blocks = out_grad.reshape(blocks, TOK_DEV, D)

    def step(total, items):
        gate_rows, up_rows, cot_rows = items
        gate_f = gate_rows.astype(jnp.float32)
        up_f = up_rows.astype(jnp.float32)
        sig = jax.nn.sigmoid(gate_f)
        act = gate_f * sig
        hidden = (act * up_f).astype(jnp.bfloat16)
        dhid = jnp.dot(cot_rows, w_down.T, preferred_element_type=jnp.float32)
        d_up = (dhid * act).astype(jnp.bfloat16)
        d_gate = (dhid * up_f * sig * (1.0 + gate_f * (1.0 - sig))).astype(jnp.bfloat16)
        total = total + jnp.dot(hidden.T, cot_rows, preferred_element_type=jnp.float32)
        return total, (d_gate, d_up)

    start = jnp.zeros((FF, D), jnp.float32)
    summed, outs = lax.scan(step, start, (gate_blocks, up_blocks, grad_blocks))
    grad_down = summed * (float(TOKENS) ** -0.5)
    row_energy = jnp.sum(grad_down * grad_down, axis=1) / D
    d_gate = outs[0].reshape(TOKENS, FF)
    d_up = outs[1].reshape(TOKENS, FF)
    return d_gate, d_up, grad_down, row_energy
```

```python
import functools

import jax
import jax.numpy as jnp
from jax import lax
from jax.experimental import pallas as pl
from jax.experimental.pallas import tpu as pltpu
from jax.sharding import PartitionSpec as P

MESH = pl.DeviceIdType.MESH
F32 = jnp.float32
BF16 = jnp.bfloat16
PIECES = 8
SPLIT = 2
LAG = 2


def plain(gate_pre, up_pre, out_grad, w_down):
    gate_f = gate_pre.astype(F32)
    up_f = up_pre.astype(F32)
    sig = jax.nn.sigmoid(gate_f)
    act = gate_f * sig
    hidden = (act * up_f).astype(BF16)
    tokens_all = out_grad.shape[0] * lax.axis_size("rep") * lax.axis_size("fs")
    factor = float(tokens_all) ** (-0.5)
    weight_whole = lax.all_gather(w_down, "fs", axis=1, tiled=True)
    dhid = lax.dot_general(out_grad, weight_whole, (((1,), (1,)), ((), ())), preferred_element_type=F32)
    d_up = (dhid * act).astype(BF16)
    d_gate = (dhid * up_f * sig * (1.0 + gate_f * (1.0 - sig))).astype(BF16)
    shard = lax.psum_scatter(
        lax.dot_general(out_grad, hidden, (((0,), (0,)), ((), ())), preferred_element_type=F32),
        "fs",
        scatter_dimension=0,
        tiled=True,
    )
    shard = lax.psum(shard, "rep")
    grad_down = shard.T * factor
    energy = lax.psum(jnp.sum(grad_down * grad_down, axis=1), "fs") / out_grad.shape[1]
    return (d_gate, d_up, grad_down, energy)


def kernel(
    n, factor, width,
    g_hbm, u_hbm, og_hbm, w_hbm,
    dg_hbm, du_hbm, gd_hbm, en_ref,
    g, u, og, dg, du, gd, w, hid, part, zsend, zrecv, ysend, yrecv, fsend, frecv, lanes, esend, erecv,
    in_sem, out_sem, gd_sem, zs_sem, zr_sem, as_sem, ar_sem, ys_sem, yr_sem, fs_sem, fr_sem, es_sem, er_sem,
):
    rep = lax.axis_index("rep")
    k = lax.axis_index("fs")
    mate = 1 - rep
    cols = w.shape[3]
    hidden_units = g.shape[1]
    tokens = g.shape[0]
    count = PIECES - SPLIT

    def piece(c):
        return c + jnp.where(c < SPLIT, rep * SPLIT, SPLIT)

    def loop(lo, hi, body):
        lax.fori_loop(lo, hi, lambda i, x: (body(i), x)[1], 0)

    in_w = pltpu.make_async_copy(w_hbm, w.at[k], in_sem.at[0])
    in_g = pltpu.make_async_copy(g_hbm, g, in_sem.at[1])
    in_u = pltpu.make_async_copy(u_hbm, u, in_sem.at[2])
    in_og = [
        pltpu.make_async_copy(og_hbm.at[:, pl.ds(j * cols, cols)], og.at[j], in_sem.at[3 + j]) for j in range(n)
    ]
    in_w.start()
    in_g.start()
    in_u.start()
    for j in range(n):
        in_og[j].start()

    barrier = pltpu.get_barrier_semaphore()
    for t in range(1, n):
        pl.semaphore_signal(barrier, inc=1, device_id={"fs": lax.rem(k + t, n)}, device_id_type=MESH)
    pl.semaphore_signal(barrier, inc=1, device_id={"rep": mate}, device_id_type=MESH)
    pl.semaphore_wait(barrier, n)
    in_w.wait()

    at = (k, n - 1 - k)
    sign = (1, -1)

    def along(d, s, c, src, dst):
        return pltpu.make_async_remote_copy(
            src_ref=src, dst_ref=dst, send_sem=zs_sem.at[d, s, c], recv_sem=zr_sem.at[d, s, c],
            device_id={"fs": k + sign[d]}, device_id_type=MESH,
        )

    def across(src, dst, send, recv):
        return pltpu.make_async_remote_copy(
            src_ref=src, dst_ref=dst, send_sem=send, recv_sem=recv,
            device_id={"rep": mate}, device_id_type=MESH,
        )

    def first(c):
        for d in range(2):

            @pl.when(at[d] < n - 1)
            def _():
                block = w.at[k, piece(c)]
                along(d, 0, c, block, block).start()

    loop(0, count, first)

    in_g.wait()
    in_u.wait()
    rows = tokens // 8

    def make_hidden(i):
        at_rows = pl.ds(pl.multiple_of(i * rows, rows), rows)
        gate = g[at_rows, :].astype(F32)
        act = gate * jax.nn.sigmoid(gate)
        h = (act * u[at_rows, :].astype(F32)).astype(BF16)
        hid[:, at_rows] = h.T

    loop(0, 8, make_hidden)
    for j in range(n):
        in_og[j].wait()

    def make_part(i):
        j = jnp.where(i % 2 == 0, n - 1 - i // 2, i // 2)
        part[j] = jnp.dot(hid[...], og[j], preferred_element_type=F32).reshape(part.shape[1:])
        ysend[j] = part[j, pl.ds(mate * SPLIT, SPLIT)].astype(BF16)
        across(ysend.at[j], yrecv.at[j], ys_sem.at[j], yr_sem.at[j]).start()

    loop(0, n, make_part)

    def pass_on(s, c):
        p = piece(c)
        for d in range(2):
            place = at[d]

            @pl.when(place > 0)
            def _():
                along(d, s - 1, c, zsend.at[d, 0, c], zrecv.at[d, 0, c]).wait_recv()

            @pl.when(s <= place)
            def _():
                block = w.at[k - sign[d] * s, p]

                @pl.when(place < n - 1)
                def _():
                    along(d, s, c, block, block).start()

                @pl.when(c < SPLIT)
                def _():
                    j = k - sign[d] * s
                    across(block, block, as_sem.at[j, c], ar_sem.at[j, c]).start()

            @pl.when(s > place)
            def _():
                j = k + sign[d] * (n - s)

                @pl.when(c == 0)
                def _():
                    across(ysend.at[j], yrecv.at[j], ys_sem.at[j], yr_sem.at[j]).wait_recv()

                @pl.when(c < SPLIT)
                def _():
                    part[j, p] += yrecv[j, jnp.minimum(c, SPLIT - 1)].astype(F32)

                if s > 1:

                    @pl.when(place > 0)
                    def _():
                        part[j, p] += zrecv[d, s - 2, c].astype(F32)

                zsend[d, s - 1, c] = part[j, p].astype(BF16)
                along(d, s, c, zsend.at[d, s - 1, c], zrecv.at[d, s - 1, c]).start()

    for s in range(1, n):
        loop(0, count, functools.partial(pass_on, s))

    def finish(c):
        p = piece(c)

        @pl.when(c == 0)
        def _():
            across(ysend.at[k], yrecv.at[k], ys_sem.at[k], yr_sem.at[k]).wait_recv()

        @pl.when(c < SPLIT)
        def _():
            part[k, p] += yrecv[k, jnp.minimum(c, SPLIT - 1)].astype(F32)

        for d in range(2):

            @pl.when(at[d] > 0)
            def _():
                along(d, n - 1, c, zsend.at[d, n - 2, c], zrecv.at[d, n - 2, c]).wait_recv()
                part[k, p] += zrecv[d, n - 2, c].astype(F32)

        fsend[c] = part[k, p].astype(BF16)
        across(fsend.at[c], frecv.at[c], fs_sem.at[c], fr_sem.at[c]).start()

    def put(p, value):
        gd[p] = value
        sq = value * value
        total = sq[:, :128]
        for b in range(1, cols // 128):
            total += sq[:, b * 128 : (b + 1) * 128]
        lanes[p] = total
        pltpu.make_async_copy(gd.at[p], gd_hbm.at[p], gd_sem.at[p]).start()

    def deliver(c):
        across(fsend.at[c], frecv.at[c], fs_sem.at[c], fr_sem.at[c]).wait_recv()

        @pl.when(c < SPLIT)
        def _():
            put(rep * SPLIT + c, fsend[c].astype(F32) * factor)
            put(mate * SPLIT + c, frecv[c].astype(F32) * factor)

        @pl.when(c >= SPLIT)
        def _():
            put(c + SPLIT, (fsend[c].astype(F32) + frecv[c].astype(F32)) * factor)

    blocks = 4
    brows = tokens // blocks

    def activations(i):
        at_rows = pl.ds(pl.multiple_of(i * brows, brows), brows)
        dhid = jnp.zeros((brows, hidden_units), F32)
        for j in range(n):
            dhid += lax.dot_general(
                og[j, at_rows, :], w[j].reshape(hidden_units, cols), (((1,), (1,)), ((), ())),
                preferred_element_type=F32,
            )
        gate = g[at_rows, :].astype(F32)
        up = u[at_rows, :].astype(F32)
        sig = jax.nn.sigmoid(gate)
        du[at_rows, :] = (dhid * (gate * sig)).astype(BF16)
        dg[at_rows, :] = (dhid * up * sig * (1.0 + gate * (1.0 - sig))).astype(BF16)
        pltpu.make_async_copy(du.at[at_rows], du_hbm.at[at_rows], out_sem.at[0, i]).start()
        pltpu.make_async_copy(dg.at[at_rows], dg_hbm.at[at_rows], out_sem.at[1, i]).start()

    def gathered(j):
        @pl.when(j != k)
        def _():
            for c in range(SPLIT):
                block = w.at[j, mate * SPLIT + c]
                across(block, block, as_sem.at[j, c], ar_sem.at[j, c]).wait_recv()

    def last(c):
        @pl.when(c < count)
        def _():
            finish(c)

        @pl.when(c == 0)
        def _():
            loop(0, n, gathered)

        @pl.when(c < blocks)
        def _():
            activations(c)

        @pl.when(c >= LAG)
        def _():
            deliver(c - LAG)

    loop(0, count + LAG, last)

    row = jnp.sum(lanes[...].reshape(hidden_units, 128).T, axis=0, keepdims=True)
    esend[...] = jnp.broadcast_to(row, esend.shape)

    def energy_copy(to, slot):
        return pltpu.make_async_remote_copy(
            src_ref=esend, dst_ref=erecv.at[slot], send_sem=es_sem.at[to], recv_sem=er_sem.at[slot],
            device_id={"fs": to}, device_id_type=MESH,
        )

    for t in range(1, n):
        energy_copy(lax.rem(k + t, n), k).start()

    def sent(c):
        for d in range(2):

            @pl.when(at[d] < n - 1)
            def _():
                for s in range(n):
                    along(d, s, c, zsend.at[d, 0, c], zrecv.at[d, 0, c]).wait_send()

        across(fsend.at[c], frecv.at[c], fs_sem.at[c], fr_sem.at[c]).wait_send()

    loop(0, count, sent)

    def sent_across(j):
        across(ysend.at[j], yrecv.at[j], ys_sem.at[j], yr_sem.at[j]).wait_send()

        @pl.when(j != k)
        def _():
            for c in range(SPLIT):
                block = w.at[j, rep * SPLIT + c]
                across(block, block, as_sem.at[j, c], ar_sem.at[j, c]).wait_send()

    loop(0, n, sent_across)

    def stored(i):
        at_rows = pl.ds(pl.multiple_of(i * brows, brows), brows)
        pltpu.make_async_copy(du.at[at_rows], du_hbm.at[at_rows], out_sem.at[0, i]).wait()
        pltpu.make_async_copy(dg.at[at_rows], dg_hbm.at[at_rows], out_sem.at[1, i]).wait()

    loop(0, blocks, stored)
    loop(0, PIECES, lambda p: pltpu.make_async_copy(gd.at[p], gd_hbm.at[p], gd_sem.at[p]).wait())

    for t in range(1, n):
        energy_copy(k, lax.rem(k + t, n)).wait_recv()
    total = jnp.zeros((8, hidden_units), F32)
    for j in range(n):
        total += jnp.where(j == k, esend[...], erecv[j])
    en_ref[...] = total[:1] * (1.0 / width)
    for t in range(1, n):
        energy_copy(lax.rem(k + t, n), k).wait_send()


def fused(n, gate_pre, up_pre, out_grad, w_down):
    tokens, units = gate_pre.shape
    width = out_grad.shape[1]
    cols = w_down.shape[1]
    rows = units // PIECES
    count = PIECES - SPLIT
    factor = float(tokens * lax.axis_size("rep") * n) ** (-0.5)
    any_spec = pl.BlockSpec(memory_space=pl.ANY)
    dma = pltpu.SemaphoreType.DMA
    d_gate, d_up, grad, energy = pl.pallas_call(
        functools.partial(kernel, n, factor, width),
        out_shape=(
            jax.ShapeDtypeStruct((tokens, units), BF16),
            jax.ShapeDtypeStruct((tokens, units), BF16),
            jax.ShapeDtypeStruct((PIECES, rows, cols), F32),
            jax.ShapeDtypeStruct((1, units), F32),
        ),
        in_specs=[any_spec] * 4,
        out_specs=(any_spec, any_spec, any_spec, pl.BlockSpec(memory_space=pltpu.VMEM)),
        scratch_shapes=[
            pltpu.VMEM((tokens, units), BF16),
            pltpu.VMEM((tokens, units), BF16),
            pltpu.VMEM((n, tokens, cols), BF16),
            pltpu.VMEM((tokens, units), BF16),
            pltpu.VMEM((tokens, units), BF16),
            pltpu.VMEM((PIECES, rows, cols), F32),
            pltpu.VMEM((n, PIECES, rows, cols), BF16),
            pltpu.VMEM((units, tokens), BF16),
            pltpu.VMEM((n, PIECES, rows, cols), F32),
            pltpu.VMEM((2, n - 1, count, rows, cols), BF16),
            pltpu.VMEM((2, n - 1, count, rows, cols), BF16),
            pltpu.VMEM((n, SPLIT, rows, cols), BF16),
            pltpu.VMEM((n, SPLIT, rows, cols), BF16),
            pltpu.VMEM((count, rows, cols), BF16),
            pltpu.VMEM((count, rows, cols), BF16),
            pltpu.VMEM((PIECES, rows, 128), F32),
            pltpu.VMEM((8, units), F32),
            pltpu.VMEM((n, 8, units), F32),
            dma((3 + n,)),
            dma((2, 4)),
            dma((PIECES,)),
            dma((2, n, count)),
            dma((2, n, count)),
            dma((n, SPLIT)),
            dma((n, SPLIT)),
            dma((n,)),
            dma((n,)),
            dma((count,)),
            dma((count,)),
            dma((n,)),
            dma((n,)),
        ],
        compiler_params=pltpu.CompilerParams(
            collective_id=0, has_side_effects=True, vmem_limit_bytes=60 * 1024 * 1024
        ),
    )(gate_pre, up_pre, out_grad, w_down.reshape(PIECES, rows, cols))
    return d_gate, d_up, grad.reshape(units, cols), energy.reshape(units)


def solution(mesh):
    reps, n = mesh.shape["rep"], mesh.shape["fs"]

    def local(gate_pre, up_pre, out_grad, w_down):
        units, cols = w_down.shape
        fits = reps == 2 and 2 <= n <= 4 and cols % 128 == 0 and units % (PIECES * 16) == 0 and units % 128 == 0
        if fits and gate_pre.shape[0] % 1024 == 0:
            return fused(n, gate_pre, up_pre, out_grad, w_down)
        return plain(gate_pre, up_pre, out_grad, w_down)

    placed = (P(("rep", "fs"), "tp"), P(("rep", "fs"), "tp"), P(("rep", "fs"), None), P("tp", "fs"))
    return jax.shard_map(
        local,
        mesh=mesh,
        in_specs=placed,
        out_specs=(P(("rep", "fs"), "tp"), P(("rep", "fs"), "tp"), P("tp", "fs"), P("tp")),
        check_vma=False,
    )
```

```python
import functools

import jax
import jax.numpy as jnp
from jax import lax
from jax.experimental import pallas as pl
from jax.experimental.pallas import tpu as pltpu
from jax.sharding import PartitionSpec as P

MESH = pl.DeviceIdType.MESH
F32 = jnp.float32
BF16 = jnp.bfloat16
PIECES = 6
SPLIT = 2
LAG = 2
VMEM_LIMIT = 52 * 1024 * 1024


def plain(gate_pre, up_pre, out_grad, w_down):
    gate_f = gate_pre.astype(F32)
    up_f = up_pre.astype(F32)
    sig = jax.nn.sigmoid(gate_f)
    act = gate_f * sig
    hidden = (act * up_f).astype(BF16)
    tokens_all = out_grad.shape[0] * lax.axis_size("rep") * lax.axis_size("fs")
    factor = float(tokens_all) ** (-0.5)
    weight_whole = lax.all_gather(w_down, "fs", axis=1, tiled=True)
    dhid = lax.dot_general(out_grad, weight_whole, (((1,), (1,)), ((), ())), preferred_element_type=F32)
    d_up = (dhid * act).astype(BF16)
    d_gate = (dhid * up_f * sig * (1.0 + gate_f * (1.0 - sig))).astype(BF16)
    shard = lax.psum_scatter(
        lax.dot_general(out_grad, hidden, (((0,), (0,)), ((), ())), preferred_element_type=F32),
        "fs",
        scatter_dimension=0,
        tiled=True,
    )
    shard = lax.psum(shard, "rep")
    grad_down = shard.T * factor
    energy = lax.psum(jnp.sum(grad_down * grad_down, axis=1), "fs") / out_grad.shape[1]
    return (d_gate, d_up, grad_down, energy)


def kernel(
    n, factor, width,
    g_hbm, u_hbm, og_hbm, w_hbm,
    dg, du, gd, en_ref,
    g, u, og, w, hid, part, zsend, zrecv, ysend, yrecv, fsend, frecv, lanes, esend, erecv,
    in_sem, zs_sem, zr_sem, as_sem, ar_sem, ys_sem, yr_sem, fs_sem, fr_sem, es_sem, er_sem,
):
    rep = lax.axis_index("rep")
    k = lax.axis_index("fs")
    mate = 1 - rep
    cols = w.shape[3]
    hidden_units = g.shape[1]
    tokens = g.shape[0]
    count = PIECES - SPLIT

    def piece(c):
        return c + jnp.where(c < SPLIT, rep * SPLIT, SPLIT)

    def loop(lo, hi, body):
        lax.fori_loop(lo, hi, lambda i, x: (body(i), x)[1], 0)

    in_w = pltpu.make_async_copy(w_hbm, w.at[k], in_sem.at[0])
    in_g = pltpu.make_async_copy(g_hbm, g, in_sem.at[1])
    in_u = pltpu.make_async_copy(u_hbm, u, in_sem.at[2])
    in_og = [
        pltpu.make_async_copy(og_hbm.at[:, pl.ds(j * cols, cols)], og.at[j], in_sem.at[3 + j]) for j in range(n)
    ]
    in_w.start()
    in_g.start()
    in_u.start()
    for j in range(n):
        in_og[j].start()

    barrier = pltpu.get_barrier_semaphore()
    for t in range(1, n):
        pl.semaphore_signal(barrier, inc=1, device_id={"fs": lax.rem(k + t, n)}, device_id_type=MESH)
    pl.semaphore_signal(barrier, inc=1, device_id={"rep": mate}, device_id_type=MESH)
    pl.semaphore_wait(barrier, n)
    in_w.wait()

    at = (k, n - 1 - k)
    sign = (1, -1)

    def along(d, s, c, src, dst):
        return pltpu.make_async_remote_copy(
            src_ref=src, dst_ref=dst, send_sem=zs_sem.at[d, s, c], recv_sem=zr_sem.at[d, s, c],
            device_id={"fs": k + sign[d]}, device_id_type=MESH,
        )

    def across(src, dst, send, recv):
        return pltpu.make_async_remote_copy(
            src_ref=src, dst_ref=dst, send_sem=send, recv_sem=recv,
            device_id={"rep": mate}, device_id_type=MESH,
        )

    def first(c):
        for d in range(2):

            @pl.when(at[d] < n - 1)
            def _():
                block = w.at[k, piece(c)]
                along(d, 0, c, block, block).start()

    loop(0, count, first)

    in_g.wait()
    in_u.wait()
    rows = tokens // 8

    def make_hidden(i):
        at_rows = pl.ds(pl.multiple_of(i * rows, rows), rows)
        gate = g[at_rows, :].astype(F32)
        act = gate * jax.nn.sigmoid(gate)
        h = (act * u[at_rows, :].astype(F32)).astype(BF16)
        hid[:, at_rows] = h.T

    loop(0, 8, make_hidden)
    for j in range(n):
        in_og[j].wait()

    def make_part(i):
        j = jnp.where(i % 2 == 0, n - 1 - i // 2, i // 2)
        part[j] = jnp.dot(hid[...], og[j], preferred_element_type=F32).reshape(part.shape[1:])
        ysend[j] = part[j, pl.ds(mate * SPLIT, SPLIT)].astype(BF16)
        across(ysend.at[j], yrecv.at[j], ys_sem.at[j], yr_sem.at[j]).start()

    loop(0, n, make_part)

    def pass_on(s, c):
        p = piece(c)
        for d in range(2):
            place = at[d]

            @pl.when(place > 0)
            def _():
                along(d, s - 1, c, zsend.at[d, 0, c], zrecv.at[d, 0, c]).wait_recv()

            @pl.when(s <= place)
            def _():
                block = w.at[k - sign[d] * s, p]

                @pl.when(place < n - 1)
                def _():
                    along(d, s, c, block, block).start()

                @pl.when(c < SPLIT)
                def _():
                    j = k - sign[d] * s
                    across(block, block, as_sem.at[j, c], ar_sem.at[j, c]).start()

            @pl.when(s > place)
            def _():
                j = k + sign[d] * (n - s)

                @pl.when(c == 0)
                def _():
                    across(ysend.at[j], yrecv.at[j], ys_sem.at[j], yr_sem.at[j]).wait_recv()

                @pl.when(c < SPLIT)
                def _():
                    part[j, p] += yrecv[j, jnp.minimum(c, SPLIT - 1)].astype(F32)

                if s > 1:

                    @pl.when(place > 0)
                    def _():
                        part[j, p] += zrecv[d, s - 2, c].astype(F32)

                zsend[d, s - 1, c] = part[j, p].astype(BF16)
                along(d, s, c, zsend.at[d, s - 1, c], zrecv.at[d, s - 1, c]).start()

    for s in range(1, n):
        loop(0, count, functools.partial(pass_on, s))

    def finish(c):
        p = piece(c)

        @pl.when(c == 0)
        def _():
            across(ysend.at[k], yrecv.at[k], ys_sem.at[k], yr_sem.at[k]).wait_recv()

        @pl.when(c < SPLIT)
        def _():
            part[k, p] += yrecv[k, jnp.minimum(c, SPLIT - 1)].astype(F32)

        for d in range(2):

            @pl.when(at[d] > 0)
            def _():
                along(d, n - 1, c, zsend.at[d, n - 2, c], zrecv.at[d, n - 2, c]).wait_recv()
                part[k, p] += zrecv[d, n - 2, c].astype(F32)

        fsend[c] = part[k, p].astype(BF16)
        across(fsend.at[c], frecv.at[c], fs_sem.at[c], fr_sem.at[c]).start()

    def put(p, value):
        gd[p] = value
        sq = value * value
        total = sq[:, :128]
        for b in range(1, cols // 128):
            total += sq[:, b * 128 : (b + 1) * 128]
        lanes[p] = total

    def deliver(c):
        across(fsend.at[c], frecv.at[c], fs_sem.at[c], fr_sem.at[c]).wait_recv()

        @pl.when(c < SPLIT)
        def _():
            put(rep * SPLIT + c, fsend[c].astype(F32) * factor)
            put(mate * SPLIT + c, frecv[c].astype(F32) * factor)

        @pl.when(c >= SPLIT)
        def _():
            put(c + SPLIT, (fsend[c].astype(F32) + frecv[c].astype(F32)) * factor)

    blocks = 4
    brows = tokens // blocks

    def activations(i):
        at_rows = pl.ds(pl.multiple_of(i * brows, brows), brows)
        dhid = jnp.zeros((brows, hidden_units), F32)
        for j in range(n):
            dhid += lax.dot_general(
                og[j, at_rows, :], w[j].reshape(hidden_units, cols), (((1,), (1,)), ((), ())),
                preferred_element_type=F32,
            )
        gate = g[at_rows, :].astype(F32)
        up = u[at_rows, :].astype(F32)
        sig = jax.nn.sigmoid(gate)
        du[at_rows, :] = (dhid * (gate * sig)).astype(BF16)
        dg[at_rows, :] = (dhid * up * sig * (1.0 + gate * (1.0 - sig))).astype(BF16)

    def gathered(j):
        @pl.when(j != k)
        def _():
            for c in range(SPLIT):
                block = w.at[j, mate * SPLIT + c]
                across(block, block, as_sem.at[j, c], ar_sem.at[j, c]).wait_recv()

    def last(c):
        @pl.when(c < count)
        def _():
            finish(c)

        @pl.when(c == 0)
        def _():
            loop(0, n, gathered)

        @pl.when(c < blocks)
        def _():
            activations(c)

        @pl.when(c >= LAG)
        def _():
            deliver(c - LAG)

    loop(0, count + LAG, last)

    row = jnp.sum(lanes[...].reshape(hidden_units, 128).T, axis=0, keepdims=True)
    esend[...] = jnp.broadcast_to(row, esend.shape)

    def energy_copy(to, slot):
        return pltpu.make_async_remote_copy(
            src_ref=esend, dst_ref=erecv.at[slot], send_sem=es_sem.at[to], recv_sem=er_sem.at[slot],
            device_id={"fs": to}, device_id_type=MESH,
        )

    for t in range(1, n):
        energy_copy(lax.rem(k + t, n), k).start()

    def sent(c):
        for d in range(2):

            @pl.when(at[d] < n - 1)
            def _():
                for s in range(n):
                    along(d, s, c, zsend.at[d, 0, c], zrecv.at[d, 0, c]).wait_send()

        across(fsend.at[c], frecv.at[c], fs_sem.at[c], fr_sem.at[c]).wait_send()

    loop(0, count, sent)

    def sent_across(j):
        across(ysend.at[j], yrecv.at[j], ys_sem.at[j], yr_sem.at[j]).wait_send()

        @pl.when(j != k)
        def _():
            for c in range(SPLIT):
                block = w.at[j, rep * SPLIT + c]
                across(block, block, as_sem.at[j, c], ar_sem.at[j, c]).wait_send()

    loop(0, n, sent_across)

    for t in range(1, n):
        energy_copy(k, lax.rem(k + t, n)).wait_recv()
    total = jnp.zeros((8, hidden_units), F32)
    for j in range(n):
        total += jnp.where(j == k, esend[...], erecv[j])
    en_ref[...] = total[:1] * (1.0 / width)
    for t in range(1, n):
        energy_copy(lax.rem(k + t, n), k).wait_send()


def write_out(dg, du, gd, en, dg_hbm, du_hbm, gd_hbm, en_out, sem):
    copies = [
        pltpu.make_async_copy(src, dst, sem.at[i])
        for i, (src, dst) in enumerate(((dg, dg_hbm), (du, du_hbm), (gd, gd_hbm)))
    ]
    for copy in copies:
        copy.start()
    en_out[...] = en[0, :]
    for copy in copies:
        copy.wait()


def fused(n, gate_pre, up_pre, out_grad, w_down):
    tokens, units = gate_pre.shape
    width = out_grad.shape[1]
    cols = w_down.shape[1]
    rows = units // PIECES
    count = PIECES - SPLIT
    factor = float(tokens * lax.axis_size("rep") * n) ** (-0.5)
    any_spec = pl.BlockSpec(memory_space=pl.ANY)
    vmem_spec = pl.BlockSpec(memory_space=pltpu.VMEM)
    dma = pltpu.SemaphoreType.DMA
    d_gate, d_up, grad, energy = pl.pallas_call(
        functools.partial(kernel, n, factor, width),
        out_shape=(
            pltpu.VMEM((tokens, units), BF16),
            pltpu.VMEM((tokens, units), BF16),
            pltpu.VMEM((PIECES, rows, cols), F32),
            pltpu.VMEM((1, units), F32),
        ),
        in_specs=[any_spec] * 4,
        out_specs=(vmem_spec,) * 4,
        scratch_shapes=[
            pltpu.VMEM((tokens, units), BF16),
            pltpu.VMEM((tokens, units), BF16),
            pltpu.VMEM((n, tokens, cols), BF16),
            pltpu.VMEM((n, PIECES, rows, cols), BF16),
            pltpu.VMEM((units, tokens), BF16),
            pltpu.VMEM((n, PIECES, rows, cols), F32),
            pltpu.VMEM((2, n - 1, count, rows, cols), BF16),
            pltpu.VMEM((2, n - 1, count, rows, cols), BF16),
            pltpu.VMEM((n, SPLIT, rows, cols), BF16),
            pltpu.VMEM((n, SPLIT, rows, cols), BF16),
            pltpu.VMEM((count, rows, cols), BF16),
            pltpu.VMEM((count, rows, cols), BF16),
            pltpu.VMEM((PIECES, rows, 128), F32),
            pltpu.VMEM((8, units), F32),
            pltpu.VMEM((n, 8, units), F32),
            dma((3 + n,)),
            dma((2, n, count)),
            dma((2, n, count)),
            dma((n, SPLIT)),
            dma((n, SPLIT)),
            dma((n,)),
            dma((n,)),
            dma((count,)),
            dma((count,)),
            dma((n,)),
            dma((n,)),
        ],
        compiler_params=pltpu.CompilerParams(
            collective_id=0, has_side_effects=True, vmem_limit_bytes=VMEM_LIMIT
        ),
    )(gate_pre, up_pre, out_grad, w_down.reshape(PIECES, rows, cols))
    return pl.pallas_call(
        write_out,
        out_shape=(
            jax.ShapeDtypeStruct((tokens, units), BF16),
            jax.ShapeDtypeStruct((tokens, units), BF16),
            jax.ShapeDtypeStruct((units, cols), F32),
            jax.ShapeDtypeStruct((units,), F32),
        ),
        in_specs=[vmem_spec] * 4,
        out_specs=(any_spec, any_spec, any_spec, vmem_spec),
        scratch_shapes=[dma((3,))],
        compiler_params=pltpu.CompilerParams(vmem_limit_bytes=4 * 1024 * 1024),
    )(d_gate, d_up, grad.reshape(units, cols), energy)


def solution(mesh):
    reps, n = mesh.shape["rep"], mesh.shape["fs"]

    def local(gate_pre, up_pre, out_grad, w_down):
        units, cols = w_down.shape
        fits = reps == 2 and 2 <= n <= 4 and cols % 128 == 0 and units % (PIECES * 16) == 0 and units % 128 == 0
        if fits and gate_pre.shape[0] % 1024 == 0:
            return fused(n, gate_pre, up_pre, out_grad, w_down)
        return plain(gate_pre, up_pre, out_grad, w_down)

    placed = (P(("rep", "fs"), "tp"), P(("rep", "fs"), "tp"), P(("rep", "fs"), None), P("tp", "fs"))
    return jax.shard_map(
        local,
        mesh=mesh,
        in_specs=placed,
        out_specs=(P(("rep", "fs"), "tp"), P(("rep", "fs"), "tp"), P("tp", "fs"), P("tp")),
        check_vma=False,
    )
```
